256 devices in a mesh: kv: 32 (over z, y), tp: 8 (over x, core).
Axes of the slice: x: 4, y: 4, z: 8, core: 2. Of those that a mesh axis runs over, the one named last changes fastest.
Arguments:
- stream: bfloat16 [24, 4096], P(None, ('kv', 'tp')), may hold values from -50 to 50
- attention_gain: float32 [4096], P(('kv', 'tp')), may hold values from 0.1 to 1.9
- query_down: bfloat16 [4096, 1536], P(('kv', 'tp')), may hold values from -0.09375 to 0.09375
- latent_down: bfloat16 [4096, 512], P(('kv', 'tp')), may hold values from -0.09375 to 0.09375
- rotary_down: bfloat16 [4096, 64], P(('kv', 'tp')), may hold values from -0.1875 to 0.1875
- query_gain: float32 [1536], replicated, may hold values from 0.1 to 1.9
- latent_gain: float32 [512], replicated, may hold values from 0.1 to 1.9
- query_content: bfloat16 [1536, 2048], P(None, 'tp'), may hold values from -0.15625 to 0.15625
- query_rotary: bfloat16 [1536, 1024], P(None, 'tp'), may hold values from -0.15625 to 0.15625
- key_absorb: bfloat16 [16, 128, 512], P('tp'), may hold values from -0.5 to 0.5
- value_absorb: bfloat16 [16, 512, 128], P('tp'), may hold values from -0.25 to 0.25
- latent_cache: bfloat16 [24, 8192, 512], P(None, 'kv'), may hold values from -1200 to 1200
- rotary_cache: bfloat16 [24, 8192, 64], P(None, 'kv'), may hold values from -5 to 5
- head_gain: float32 [2048], P('tp'), may hold values from 0.1 to 1.9
- output_weight: bfloat16 [2048, 4096], P('tp', 'kv'), may hold values from -0.125 to 0.125
- mixer_gain: float32 [4096], P('kv'), may hold values from 0.1 to 1.9
- gate_weight: bfloat16 [4096, 11264], P('kv', 'tp'), may hold values from -0.09375 to 0.09375
- up_weight: bfloat16 [4096, 11264], P('kv', 'tp'), may hold values from -0.09375 to 0.09375
- down_weight: bfloat16 [11264, 4096], P('tp', 'kv'), may hold values from -0.0546875 to 0.0546875
Outputs:
- stream_out: bfloat16 [24, 4096], P(None, ('kv', 'tp'))
The draws below stay inside these ranges and needn't reach their ends.
All inputs are finite; a program needn't handle non-finite values.
Results may differ from the reference program's by a relative error of at most 0.018.
Values may be sent and summed in bfloat16 or wider, within the bound.
No kernel may reach another device: no remote copies, remote signals or barrier semaphores. Data moves between devices by JAX's collectives and lax.ppermute only.
A program may use at most 64 MiB of HBM per device.

```python
import jax
import jax.numpy as jnp
from jax import lax

D = 4096
HEADS = 16
QRANK = 1536
KVRANK = 512
NOPE = 128
ROPE = 64
VDIM = 128
FF = 11264
SEQS = 24
POS_DEV = 256
LENGTH = 8192
N_KV = 32
N_TP = 8


def draw_stream(key, part):
    keys = jax.random.split(key, 3)
    columns = jnp.arange(D, dtype=jnp.float32) / D
    column_scale = jnp.exp(jnp.log(3.0) * columns + jax.random.uniform(keys[1], (1, D), jnp.float32, -0.35, 0.35))
    row_scale = jnp.exp(jax.random.uniform(keys[2], (SEQS, 1), jnp.float32, jnp.log(0.5), jnp.log(2.0)))
    entries = jax.random.truncated_normal(keys[0], -5.0, 5.0, (SEQS, D), jnp.float32)
    return (entries * row_scale * column_scale).astype(jnp.bfloat16)


def draw_latent_cache(key, part):
    keys = jax.random.split(key, 1)
    length = POS_DEV * N_KV
    base = 0.3 * jax.random.truncated_normal(keys[0], -5.0, 5.0, (SEQS, length, KVRANK), jnp.float32)
    return base.astype(jnp.bfloat16)


def block_scale(own_key, dims, pieces, low, top_value):
    factor_of, own = 1.0, jax.random.fold_in(own_key, 6)
    for dim, blocks in pieces:
        heights = jnp.exp(jax.random.uniform(jax.random.fold_in(own, dim), (blocks,), jnp.float32, low / len(pieces), top_value / len(pieces)))
        factor_of = factor_of * jnp.repeat(heights, dims[dim] // blocks).reshape([-1 if axis == dim else 1 for axis in range(len(dims))])
    return factor_of


def gaussian(stream_key, extent, scale, most, shards=(), held_as=jnp.bfloat16):
    array = scale * jax.random.normal(stream_key, extent, jnp.float32)
    if shards:
        array = array * block_scale(stream_key, extent, shards, -0.22, 0.18)
    return jnp.clip(array, -most, most).astype(held_as)


def setup_inputs(seed: int = 0) -> dict:
    streams_of = jax.random.split(jax.random.key(seed), 20)
    stream = draw_stream(jax.random.fold_in(streams_of[19], 71), 0)
    attention_gain = jnp.clip(1.0 + 0.18 * jax.random.normal(streams_of[1], (D,), jnp.float32), 0.1, 1.9)
    query_down = gaussian(streams_of[2], (D, QRANK), D ** -0.5, 0.09375, ((0, 256),))
    latent_down = gaussian(streams_of[3], (D, KVRANK), D ** -0.5, 0.09375, ((0, 256),))
    rotary_down = gaussian(streams_of[4], (D, ROPE), (D // 4) ** -0.5, 0.1875, ((0, 256),))
    query_gain = jnp.clip(1.0 + 0.18 * jax.random.normal(streams_of[5], (QRANK,), jnp.float32), 0.1, 1.9)
    latent_gain = jnp.clip(1.0 + 0.18 * jax.random.normal(streams_of[6], (KVRANK,), jnp.float32), 0.1, 1.9)
    query_content = gaussian(streams_of[7], (QRANK, HEADS * NOPE), QRANK ** -0.5, 0.15625, ((1, 8),))
    query_rotary = gaussian(streams_of[8], (QRANK, HEADS * ROPE), QRANK ** -0.5, 0.15625, ((1, 8),))
    key_absorb = gaussian(streams_of[9], (HEADS, NOPE, KVRANK), NOPE ** -0.5, 0.5, ((0, 8),))
    value_absorb = gaussian(streams_of[10], (HEADS, KVRANK, VDIM), KVRANK ** -0.5, 0.25, ((0, 8),))
    latent_cache = draw_latent_cache(jax.random.fold_in(streams_of[19], 71), 0)
    rotary_cache = gaussian(streams_of[12], (SEQS, LENGTH, ROPE), 1.0, 5.0, ((1, 32),))
    head_gain = jnp.clip(1.0 + 0.18 * jax.random.normal(streams_of[13], (HEADS * VDIM,), jnp.float32), 0.1, 1.9)
    output_weight = gaussian(streams_of[14], (HEADS * VDIM, D), (HEADS * VDIM) ** -0.5, 0.125, ((0, 8), (1, 32)))
    mixer_gain = jnp.clip(1.0 + 0.18 * jax.random.normal(streams_of[15], (D,), jnp.float32), 0.1, 1.9)
    gate_weight = gaussian(streams_of[16], (D, FF), D ** -0.5, 0.09375, ((0, 32), (1, 8)))
    up_weight = gaussian(streams_of[17], (D, FF), D ** -0.5, 0.09375, ((0, 32), (1, 8)))
    down_weight = gaussian(streams_of[18], (FF, D), FF ** -0.5, 0.0546875, ((0, 8), (1, 32)))
    return {"stream": stream, "attention_gain": attention_gain, "query_down": query_down, "latent_down": latent_down, "rotary_down": rotary_down, "query_gain": query_gain, "latent_gain": latent_gain, "query_content": query_content, "query_rotary": query_rotary, "key_absorb": key_absorb, "value_absorb": value_absorb, "latent_cache": latent_cache, "rotary_cache": rotary_cache, "head_gain": head_gain, "output_weight": output_weight, "mixer_gain": mixer_gain, "gate_weight": gate_weight, "up_weight": up_weight, "down_weight": down_weight}


epsilon = 1e-06
rope_base = 10000.0

def rotate(values, position):
    half = values.shape[-1] // 2
    freqs = rope_base ** (-jnp.arange(half, dtype=jnp.float32) * 2.0 / values.shape[-1])
    angle = position * freqs
    cosine = jnp.cos(angle)
    sine = jnp.sin(angle)
    first = values[..., :half]
    second = values[..., half:]
    return jnp.concatenate([first * cosine - second * sine, second * cosine + first * sine], axis=-1)

def inv_rms(values):
    return lax.rsqrt(lax.optimization_barrier(jnp.mean(values * values, axis=-1)) + epsilon)

def block_sum(left, right, parts):
    rows = left.shape[0]
    inner = right.shape[0] // parts
    terms = jnp.einsum('btf,tfd->btd', left.reshape(rows, parts, inner).astype(jnp.float32), right.reshape(parts, inner, right.shape[1]).astype(jnp.float32))
    rounded = lax.optimization_barrier(terms.astype(jnp.bfloat16))
    return lax.optimization_barrier(jnp.sum(rounded.astype(jnp.float32), axis=1))

def reference(stream, attention_gain, query_down, latent_down, rotary_down, query_gain, latent_gain, query_content, query_rotary, key_absorb, value_absorb, latent_cache, rotary_cache, head_gain, output_weight, mixer_gain, gate_weight, up_weight, down_weight):
    batch_rows = stream.shape[0]
    length = latent_cache.shape[1]
    position = jnp.float32(length)
    stream_f = stream.astype(jnp.float32)
    first_scale = inv_rms(stream_f)[:, None]
    first_scaled = (stream_f * attention_gain).astype(jnp.bfloat16)
    query_low = first_scale * jnp.dot(first_scaled, query_down, preferred_element_type=jnp.float32)
    latent_new = first_scale * jnp.dot(first_scaled, latent_down, preferred_element_type=jnp.float32)
    rotary_new = first_scale * jnp.dot(first_scaled, rotary_down, preferred_element_type=jnp.float32)
    query_normed = (query_low * inv_rms(query_low)[:, None] * query_gain).astype(jnp.bfloat16)
    latent_row = (latent_new * inv_rms(latent_new)[:, None] * latent_gain).astype(jnp.bfloat16)
    rotary_row = rotate(rotary_new, position).astype(jnp.bfloat16)
    heads = key_absorb.shape[0]
    query_plain = jnp.dot(query_normed, query_content, preferred_element_type=jnp.float32).astype(jnp.bfloat16)
    query_plain = query_plain.reshape(batch_rows, heads, key_absorb.shape[1])
    query_turned = jnp.dot(query_normed, query_rotary, preferred_element_type=jnp.float32)
    query_turned = rotate(query_turned.reshape(batch_rows, heads, rotary_cache.shape[2]), position).astype(jnp.bfloat16)
    query_latent = jnp.einsum('bhn,hnc->bhc', query_plain.astype(jnp.float32), key_absorb.astype(jnp.float32)).astype(jnp.bfloat16)
    scale = (key_absorb.shape[1] + rotary_cache.shape[2]) ** (-0.5)
    blocks = length // POS_DEV

    def one_sequence(items):
        row_latent, row_turned, latents, rotaries = items
        scores = (jnp.dot(row_latent, latents.T, preferred_element_type=jnp.float32) + jnp.dot(row_turned, rotaries.T, preferred_element_type=jnp.float32)) * scale
        scores = scores.reshape(heads, blocks, POS_DEV)
        maxima = lax.optimization_barrier(jnp.max(scores, axis=-1))
        expo = jnp.exp(scores - maxima[..., None])
        totals = lax.optimization_barrier(jnp.sum(expo, axis=-1))
        weights = expo.astype(jnp.bfloat16)
        weighted = jnp.einsum('hnp,npc->hnc', weights.astype(jnp.float32), latents.reshape(blocks, POS_DEV, latents.shape[1]).astype(jnp.float32))
        return (maxima, totals, weighted.astype(jnp.bfloat16))
    maxima, totals, weighted = lax.map(one_sequence, (query_latent, query_turned, latent_cache, rotary_cache))
    own_score = (lax.optimization_barrier(jnp.sum(query_latent.astype(jnp.float32) * latent_row.astype(jnp.float32)[:, None, :], axis=-1)) + lax.optimization_barrier(jnp.sum(query_turned.astype(jnp.float32) * rotary_row.astype(jnp.float32)[:, None, :], axis=-1))) * scale
    largest = jnp.maximum(lax.optimization_barrier(jnp.max(maxima, axis=-1)), own_score)
    factors = jnp.exp(maxima - largest[..., None])
    own_weight = jnp.exp(own_score - largest)
    denominator = lax.optimization_barrier(jnp.sum(factors * totals, axis=-1)) + own_weight
    merged = lax.optimization_barrier(jnp.sum(factors[..., None] * weighted.astype(jnp.float32), axis=2))
    merged = merged + own_weight[..., None] * latent_row.astype(jnp.float32)[:, None, :]
    latent_mix = (merged / denominator[..., None]).astype(jnp.bfloat16)
    head_values = jnp.einsum('bhc,hcv->bhv', latent_mix.astype(jnp.float32), value_absorb.astype(jnp.float32)).astype(jnp.bfloat16)
    head_f = head_values.reshape(batch_rows, heads * value_absorb.shape[2]).astype(jnp.float32)
    head_scale = inv_rms(head_f)[:, None]
    head_scaled = (head_f * head_gain).astype(jnp.bfloat16)
    attended = block_sum(head_scaled, output_weight, N_TP)
    middle = (stream_f + head_scale * attended).astype(jnp.bfloat16)
    middle_f = middle.astype(jnp.float32)
    second_scale = inv_rms(middle_f)[:, None]
    second_scaled = (middle_f * mixer_gain).astype(jnp.bfloat16)
    gate = second_scale * jnp.dot(second_scaled, gate_weight, preferred_element_type=jnp.float32)
    up = second_scale * jnp.dot(second_scaled, up_weight, preferred_element_type=jnp.float32)
    hidden = (jax.nn.silu(gate) * up).astype(jnp.bfloat16)
    mixed = block_sum(hidden, down_weight, N_TP)
    return (middle_f + mixed).astype(jnp.bfloat16)
```

```python
import functools
import math

import jax
import jax.numpy as jnp
import numpy as np
from jax import lax
from jax.experimental import pallas as pl
from jax.experimental.pallas import tpu as pltpu
from jax.sharding import Mesh
from jax.sharding import PartitionSpec as P

KV, TP = ("z", "yh", "yl"), ("x", "c")
NEAR, FAR = ("yl", "x", "c"), ("z", "yh")
EPS = 1e-06
BASE = 10000.0
MIB = 1 << 20
F32, BF16 = jnp.float32, jnp.bfloat16
NT = (((1,), (1,)), ((), ()))


def mm(a, b):
    return jnp.dot(a, b, preferred_element_type=F32)


def mm_nt(a, b):
    return lax.dot_general(a, b, NT, preferred_element_type=F32)


def diagonal(rows, lanes):
    r = lax.broadcasted_iota(jnp.int32, (rows, lanes), 0)
    return r == lax.broadcasted_iota(jnp.int32, (rows, lanes), 1)


def as_row(col, lanes=128):
    return jnp.sum(jnp.where(diagonal(col.shape[0], lanes), col, 0.0), axis=0, keepdims=True)


def as_col(row, n):
    return jnp.sum(jnp.where(diagonal(n, row.shape[1]), row, 0.0), axis=1, keepdims=True)


def parts_of(x, count):
    out = []
    for _ in range(count):
        top = x.astype(BF16).astype(F32)
        out.append(top)
        x = x - top
    return out


def stacked(rows, lanes=128):
    index = lax.broadcasted_iota(jnp.int32, (8, lanes), 0)
    tile = jnp.zeros((8, lanes), F32)
    for k, row in enumerate(rows):
        tile = jnp.where(index == k, row, tile)
    return tile


def call(body, out, ins, scratch=(), mib=8, flops=1000000, hbm=()):
    single = not isinstance(out, list)
    outs = [out] if single else list(out)
    ins = [pltpu.with_memory_space_constraint(x, pltpu.HBM) if k in hbm else x for k, x in enumerate(ins)]
    got = pl.pallas_call(
        body,
        out_shape=[pltpu.VMEM(s, d) if hbm else jax.ShapeDtypeStruct(s, d) for s, d in outs],
        in_specs=[pl.BlockSpec(memory_space=pltpu.HBM if k in hbm else pltpu.VMEM) for k in range(len(ins))],
        out_specs=[pl.BlockSpec(memory_space=pltpu.VMEM)] * len(outs),
        scratch_shapes=list(scratch),
        compiler_params=pltpu.CompilerParams(vmem_limit_bytes=mib * MIB),
        cost_estimate=pl.CostEstimate(flops=flops, bytes_accessed=100000, transcendentals=0),
    )(*ins)
    return got[0] if single else got


def compress(
    rows, stream_hbm, gain_hbm, query_hbm, latent_hbm, rotary_hbm,
    out_ref, stream_ref, gain_ref, query_ref, latent_ref, rotary_ref, sems,
):
    copies = [
        pltpu.make_async_copy(a, b, sems.at[k])
        for k, (a, b) in enumerate((
            (stream_hbm, stream_ref), (gain_hbm, gain_ref), (rotary_hbm, rotary_ref),
            (latent_hbm, latent_ref), (query_hbm, query_ref),
        ))
    ]
    for copy in copies:
        copy.start()
    for copy in copies:
        copy.wait()
    own_f = mm_nt(diagonal(rows, rows).astype(BF16), stream_ref[...])
    own = own_f.astype(BF16)
    scaled = (own_f * gain_ref[...]).astype(BF16)
    query = mm(scaled, query_ref[...])
    latent = mm(scaled, latent_ref[...])
    rotary = mm(scaled, rotary_ref[...]).astype(BF16)
    wide = rotary.shape[1]
    turned = mm_nt(diagonal(wide, wide).astype(BF16), rotary)
    square = jnp.broadcast_to(as_row(jnp.sum(own_f * own_f, axis=1, keepdims=True)), (8, 128)).astype(BF16)
    count = own.shape[1]
    chunks = out_ref.shape[0]
    piece = wide // chunks
    for j in range(chunks):
        at = 128 * j
        part = query[:, at : at + 128] if at < query.shape[1] else latent[:, at - query.shape[1] : at - query.shape[1] + 128]
        out_ref[j, :rows, :] = part.astype(BF16)
        out_ref[j, rows:, :] = square
        out_ref[j, rows : rows + piece, :rows] = turned[piece * j : piece * (j + 1), :].astype(BF16)
        for g in range(rows // 8):
            out_ref[j, rows:, 32 + count * g : 32 + count * (g + 1)] = own[8 * g : 8 * g + 8, :]


def total_of(in_ref):
    total = in_ref[0].astype(F32)
    for p in range(1, in_ref.shape[0]):
        total += in_ref[p].astype(F32)
    return total


def first_sum(rows, count, in_ref, out_ref, block_ref):
    total = total_of(in_ref).astype(BF16)
    for k in range(out_ref.shape[0]):
        out_ref[k] = total
    peers = block_ref.shape[1] // count
    base = peers * lax.axis_index("yl")
    for p in range(peers):
        for g in range(rows // 8):
            block_ref[8 * g : 8 * g + 8, count * p : count * (p + 1)] = in_ref[base + p, rows:, 32 + count * g : 32 + count * (g + 1)]


def plain_sum(in_ref, out_ref):
    total = total_of(in_ref).astype(BF16)
    for k in range(out_ref.shape[0]):
        out_ref[k] = total


def fetch(count, token_ref, *refs):
    sources, targets, sems = refs[:count], refs[count:-1], refs[-1]
    copies = [pltpu.make_async_copy(a, b, sems.at[k]) for k, (a, b) in enumerate(zip(sources, targets))]
    for copy in copies:
        copy.start()
    for copy in copies:
        copy.wait()


def attend(
    rows, width, scale,
    in_ref, qgain_ref, lgain_ref, trig_ref,
    content_ref, rotary_ref, key_ref, value_ref, turned_ref, latents_hbm,
    out_ref, q_ref, qt_ref, s_ref, w_ref, r_ref, latents_ref, sems,
):
    group = rows // sems.shape[0]
    copies = [
        pltpu.make_async_copy(latents_hbm.at[group * k : group * (k + 1)], latents_ref.at[group * k : group * (k + 1)], sems.at[k])
        for k in range(sems.shape[0])
    ]
    for copy in copies:
        copy.start()
    heads = key_ref.shape[0]
    extent = turned_ref.shape[1]
    half = extent // 2
    pieces = q_ref.shape[0]
    chunks = in_ref.shape[0]
    n_query = qgain_ref.shape[0]
    eye = diagonal(rows, 128)
    part = extent // chunks
    first_row = lax.rsqrt(in_ref[0, rows + part : rows + part + 1, :].astype(F32) / width + EPS)
    first = as_col(first_row, rows)

    def normed_of(tiles, gain_ref):
        tiles = [in_ref[j, :rows, :].astype(F32) * first for j in tiles]
        square = jnp.sum(sum(x * x for x in tiles), axis=1, keepdims=True)
        inverse = lax.rsqrt(square / (128 * len(tiles)) + EPS)
        return jnp.concatenate([x * inverse * gain_ref[j : j + 1, :] for j, x in enumerate(tiles)], axis=1).astype(BF16)

    normed = normed_of(range(n_query), qgain_ref)
    row = normed_of(range(n_query, chunks), lgain_ref).astype(F32)
    for j in range(chunks):
        r_ref[part * j : part * (j + 1), :] = in_ref[j, rows : rows + part, :].astype(F32) * first_row
    low_half, high_half = r_ref[:half, :], r_ref[half:extent, :]
    cos_t, sin_t = trig_ref[:half, :], trig_ref[half : 2 * half, :]
    spun = jnp.concatenate([low_half * cos_t - high_half * sin_t, high_half * cos_t + low_half * sin_t], axis=0).astype(BF16)

    plain = mm(normed, content_ref[...]).astype(BF16)
    turn = mm(normed, rotary_ref[...])
    lane = lax.broadcasted_iota(jnp.int32, turn.shape, 1)
    across = turn.shape[1]
    swapped = jnp.where(lane % extent < half, pltpu.roll(turn, across - half, 1), pltpu.roll(turn, half, 1))
    turn = (turn * trig_ref[2 * half : 2 * half + 1, :] + swapped * trig_ref[2 * half + 1 : 2 * half + 2, :]).astype(BF16)
    turn_f = turn.astype(F32)

    q_ref[...] = jnp.zeros_like(q_ref)
    qt_ref[...] = jnp.zeros_like(qt_ref)
    own = []
    for h in range(heads):
        absorbed = mm(plain[:, 128 * h : 128 * h + 128], key_ref[h]).astype(BF16).astype(F32)
        for c in range(pieces):
            q_ref[c, pl.ds(h, rows, 8), :] = absorbed[:, 128 * c : 128 * c + 128]
        qt_ref[pl.ds(h, rows, 8), :] = turn_f if h == 0 else pltpu.roll(turn_f, across - extent * h, 1)
        turned_h = turn[:, extent * h : extent * (h + 1)]
        cross = jnp.sum(jnp.where(eye, mm(turned_h, spun), 0.0), axis=1, keepdims=True)
        own.append((jnp.sum(absorbed * row, axis=1, keepdims=True) + cross) * scale)

    for b in range(rows):
        if b % group == 0:
            copies[b // group].wait()
        at = slice(8 * b, 8 * b + 8)
        asked = jnp.concatenate([q_ref[c, at, :] for c in range(pieces)], axis=1).astype(BF16)
        s_ref[at, :] = (mm_nt(asked, latents_ref[b]) + mm(qt_ref[at, :extent].astype(BF16), turned_ref[b])) * scale
    scores = s_ref[...]
    tops = jnp.max(scores, axis=1, keepdims=True)
    expo = jnp.exp(scores - tops)
    s_ref[...] = expo
    r_ref[: 8 * rows, :] = jnp.broadcast_to(tops, (8 * rows, 128))
    r_ref[8 * rows :, :] = jnp.broadcast_to(jnp.sum(expo, axis=1, keepdims=True), (8 * rows, 128))
    for b in range(rows):
        at = slice(8 * b, 8 * b + 8)
        weighted = mm(s_ref[at, :].astype(BF16), latents_ref[b])
        for c in range(pieces):
            w_ref[c, at, :] = weighted[:, 128 * c : 128 * c + 128]

    here = lax.axis_index(KV) == 0
    values, logs = [], []
    for h in range(heads):
        weighted = jnp.concatenate([w_ref[c, pl.ds(h, rows, 8), :] for c in range(pieces)], axis=1)
        top = r_ref[pl.ds(h, rows, 8), :][:, :1]
        total = r_ref[pl.ds(8 * rows + h, rows, 8), :][:, :1]
        mine = jnp.where(here, own[h], -1e30)
        peak = jnp.maximum(top, mine)
        keep = jnp.exp(top - peak)
        add = jnp.exp(mine - peak)
        total = total * keep + add
        mixed = ((weighted * keep + row * add) / total).astype(BF16)
        values.append(mm(mixed, value_ref[h]).astype(BF16))
        logs += parts_of(as_row(peak + jnp.log(total)), 3)
    tile = stacked(logs).astype(BF16)
    for k in range(out_ref.shape[0]):
        for h in range(heads):
            out_ref[k, rows * h : rows * (h + 1), :] = values[h]
        out_ref[k, rows * heads :, :] = tile


def project(rows, in_ref, gain_ref, weight_ref, out_ref):
    blocks = in_ref.shape[0]
    heads = in_ref.shape[1] // rows
    logs = []
    for k in range(blocks):
        tile = in_ref[k, rows * heads :, :].astype(F32)
        logs.append(tile + pltpu.roll(tile, 7, 0) + pltpu.roll(tile, 6, 0))
    peak = functools.reduce(jnp.maximum, logs)
    factors = [jnp.exp(x - peak) for x in logs]
    whole = 1.0 / functools.reduce(jnp.add, factors)
    spread = jnp.concatenate([x * whole for x in factors], axis=0)
    eye = diagonal(rows, 128).astype(BF16)
    columns = sum(mm_nt(eye, x.astype(BF16)) for x in parts_of(spread, 2))
    values = []
    for h in range(heads):
        total = jnp.zeros((rows, 128), F32)
        for k in range(blocks):
            total += columns[:, 8 * k + 3 * h : 8 * k + 3 * h + 1] * in_ref[k, rows * h : rows * (h + 1), :].astype(F32)
        values.append(total.astype(BF16).astype(F32))
    values = jnp.concatenate(values, axis=1)
    square = as_row(jnp.sum(values * values, axis=1, keepdims=True))
    scaled = (values * gain_ref[...]).astype(BF16)
    product = mm(scaled, weight_ref[...]).astype(BF16)
    tile = stacked(parts_of(square, 2)).astype(BF16)
    for p in range(out_ref.shape[0]):
        out_ref[p, :rows, :] = product
        out_ref[p, rows:, :] = tile


def spots(rows, tiles):
    return [(8 * (t // tiles), 128 * (t % tiles)) for t in range(rows // 8 * tiles)]


def expand(rows, width, in_ref, block_ref, gain_ref, gate_ref, up_ref, out_ref, middle_ref):
    attended = total_of(in_ref)
    head_row = lax.rsqrt((attended[rows : rows + 1] + attended[rows + 1 : rows + 2]) / width + EPS)
    middle = (block_ref[...].astype(F32) + as_col(head_row, rows) * attended[:rows]).astype(BF16)
    middle_ref[...] = middle
    middle = middle.astype(F32)
    square = as_row(jnp.sum(middle * middle, axis=1, keepdims=True))
    tile = stacked(parts_of(square, 2)).astype(BF16)
    scaled = (middle * gain_ref[...]).astype(BF16)
    places = spots(rows, gate_ref.shape[1] // 128)
    owners = out_ref.shape[0]
    spare = len(places) - owners
    for at, weight_ref in ((0, gate_ref), (8, up_ref)):
        product = mm(scaled, weight_ref[...])
        for t in range(owners):
            for slot, (r, c) in enumerate([places[t]] + places[owners:]):
                out_ref[t, 16 * slot + at : 16 * slot + at + 8, :] = product[r : r + 8, c : c + 128].astype(BF16)
    for t in range(owners):
        out_ref[t, 16 * (1 + spare) :, :] = tile


def activate(rows, width, tiles, in_ref, out_ref, rest_ref, scale_ref):
    total = total_of(in_ref)
    owners = out_ref.shape[0]
    places = spots(rows, tiles)
    spare = len(places) - owners
    last = 16 * (1 + spare)
    scale_row = lax.rsqrt((total[last : last + 1] + total[last + 1 : last + 2]) / width + EPS)
    scale_ref[...] = jnp.broadcast_to(as_col(scale_row, rows), scale_ref.shape)

    def hidden(slot, scale):
        gate = total[16 * slot : 16 * slot + 8] * scale
        up = total[16 * slot + 8 : 16 * slot + 16] * scale
        return (gate / (1.0 + jnp.exp(-gate)) * up).astype(BF16)

    group = lax.axis_index(KV) // tiles
    mine = hidden(0, scale_ref[pl.ds(pl.multiple_of(8 * group, 8), 8), :])
    for k in range(owners):
        out_ref[k] = mine
    for s in range(spare):
        r, _ = places[owners + s]
        rest_ref[8 * s : 8 * s + 8, :] = hidden(1 + s, scale_ref[r : r + 8, :])


def contract(rows, tiles, in_ref, rest_ref, weight_ref, out_ref, hidden_ref):
    owners = in_ref.shape[0]
    for t, (r, c) in enumerate(spots(rows, tiles)):
        part = in_ref[t] if t < owners else rest_ref[8 * (t - owners) : 8 * (t - owners) + 8, :]
        hidden_ref[r : r + 8, c : c + 128] = part
    product = mm(hidden_ref[...], weight_ref[...]).astype(BF16)
    for p in range(out_ref.shape[0]):
        out_ref[p] = product


def finish(in_ref, middle_ref, out_ref):
    total = (middle_ref[...].astype(F32) + total_of(in_ref)).astype(BF16)
    width = out_ref.shape[0]
    at = (width, total.shape[1])
    row = lax.broadcasted_iota(jnp.int32, at, 0) + width * lax.axis_index(TP)
    pick = (row == lax.broadcasted_iota(jnp.int32, at, 1)).astype(BF16)
    out_ref[...] = mm_nt(pick, total).astype(BF16)


def exchange(x, axis):
    return lax.all_to_all(x, axis, 0, 0, tiled=True)


def local(
    stream, attention_gain, query_down, latent_down, rotary_down, query_gain, latent_gain,
    query_content, query_rotary, key_absorb, value_absorb, latent_cache, rotary_cache,
    head_gain, output_weight, mixer_gain, gate_weight, up_weight, down_weight,
):
    kv, tp = lax.axis_size(KV), lax.axis_size(TP)
    near, far = lax.axis_size(NEAR), lax.axis_size(FAR)
    rows, count = stream.shape
    width = count * kv * tp
    heads, nope, latent = key_absorb.shape
    rope = rotary_cache.shape[2]
    block_len = latent_cache.shape[1]
    position = block_len * kv
    scale = (nope + rope) ** (-0.5)
    tiles = gate_weight.shape[1] // 128
    spare = rows // 8 * tiles - kv
    angle = position * BASE ** (-np.arange(rope // 2) * 2.0 / rope)
    cos, sin = np.cos(angle), np.sin(angle)
    trig = np.concatenate([
        np.tile(cos[:, None], (1, 128)), np.tile(sin[:, None], (1, 128)),
        np.tile(np.concatenate([cos, cos]), heads)[None], np.tile(np.concatenate([-sin, sin]), heads)[None],
        np.zeros((6, 128)),
    ])
    trig = jnp.asarray(trig, F32)
    lines = rows + 8

    sources = (stream.T, attention_gain[None], query_down, latent_down, rotary_down)
    sent = call(
        functools.partial(compress, rows), ((near, lines, 128), BF16), sources,
        scratch=[pltpu.VMEM(x.shape, x.dtype) for x in sources] + [pltpu.SemaphoreType.DMA((len(sources),))],
        hbm=range(len(sources)),
    )
    sent, block = call(
        functools.partial(first_sum, rows, count), [((far, lines, 128), BF16), ((rows, count * tp), BF16)],
        (exchange(sent, NEAR),),
    )
    sources = (
        query_gain.reshape(-1, 128), latent_gain.reshape(-1, 128), trig,
        query_content, query_rotary, key_absorb, value_absorb, jnp.swapaxes(rotary_cache, 1, 2),
    )
    held = call(
        functools.partial(fetch, len(sources)), [(x.shape, x.dtype) for x in sources], (block, *sources),
        scratch=[pltpu.SemaphoreType.DMA((len(sources),))], hbm=range(1, len(sources) + 1), flops=20000000,
    )
    sent = call(plain_sum, ((near, lines, 128), BF16), (exchange(sent, FAR),))
    sent = call(
        functools.partial(attend, rows, width, scale), ((kv, rows * heads + 8, 128), BF16),
        (exchange(sent, NEAR), *held, latent_cache),
        scratch=[
            pltpu.VMEM((latent // 128, 8 * rows, 128), F32), pltpu.VMEM((8 * rows, heads * rope), F32),
            pltpu.VMEM((8 * rows, block_len), F32), pltpu.VMEM((latent // 128, 8 * rows, 128), F32),
            pltpu.VMEM((16 * rows, 128), F32), pltpu.VMEM(latent_cache.shape, BF16), pltpu.SemaphoreType.DMA((4,)),
        ],
        mib=24, hbm=(1 + len(held),),
    )
    sent = call(
        functools.partial(project, rows), ((tp, lines, 128), BF16),
        (exchange(sent, KV), head_gain[None], output_weight),
    )
    sent, middle = call(
        functools.partial(expand, rows, head_gain.shape[0] * tp),
        [((kv, 16 * (1 + spare) + 8, 128), BF16), ((rows, 128), BF16)],
        (exchange(sent, TP), block, mixer_gain[None], gate_weight, up_weight),
    )
    sent, rest = call(
        functools.partial(activate, rows, width, tiles), [((kv, 8, 128), BF16), ((8 * spare, 128), BF16)],
        (exchange(sent, KV),), scratch=[pltpu.VMEM((rows, 128), F32)],
    )
    sent = call(
        functools.partial(contract, rows, tiles), ((tp, rows, 128), BF16),
        (exchange(sent, KV), rest, down_weight), scratch=[pltpu.VMEM((rows, 128 * tiles), BF16)],
    )
    return call(finish, ((count, rows), BF16), (exchange(sent, TP), middle)).T


def solution(mesh):
    grid = Mesh(mesh.devices.reshape(mesh.shape["kv"] // 4, 2, 2, mesh.shape["tp"] // 2, 2), KV + TP)
    both = KV + TP
    return jax.shard_map(
        local,
        mesh=grid,
        in_specs=(
            P(None, both), P(both), P(both, None), P(both, None), P(both, None), P(), P(),
            P(None, TP), P(None, TP), P(TP, None, None), P(TP, None, None),
            P(None, KV, None), P(None, KV, None), P(TP), P(TP, KV), P(KV),
            P(KV, TP), P(KV, TP), P(TP, KV),
        ),
        out_specs=P(None, both),
        check_vma=False,
    )
```

```python
import functools
import math

import jax
import jax.numpy as jnp
import numpy as np
from jax import lax
from jax.experimental import pallas as pl
from jax.experimental.pallas import tpu as pltpu
from jax.sharding import Mesh
from jax.sharding import PartitionSpec as P

KV, TP = ("z", "yh", "yl"), ("x", "c")
NEAR, FAR = ("yl", "x", "c"), ("z", "yh")
ALONG_KV, ALONG_Y = ("yh", "yl", "z"), ("yh", "yl")
SPOT = 32
EPS = 1e-06
WAIT = 10000000000
BASE = 10000.0
MIB = 1 << 20
F32, BF16 = jnp.float32, jnp.bfloat16
NT = (((1,), (1,)), ((), ()))


def mm(a, b):
    return jnp.dot(a, b, preferred_element_type=F32)


def mm_nt(a, b):
    return lax.dot_general(a, b, NT, preferred_element_type=F32)


def diagonal(rows, lanes):
    r = lax.broadcasted_iota(jnp.int32, (rows, lanes), 0)
    return r == lax.broadcasted_iota(jnp.int32, (rows, lanes), 1)


def as_row(col, lanes=128):
    return jnp.sum(jnp.where(diagonal(col.shape[0], lanes), col, 0.0), axis=0, keepdims=True)


def as_col(row, n):
    return jnp.sum(jnp.where(diagonal(n, row.shape[1]), row, 0.0), axis=1, keepdims=True)


def parts_of(x, count):
    out = []
    for _ in range(count):
        top = x.astype(BF16).astype(F32)
        out.append(top)
        x = x - top
    return out


def stacked(rows, lanes=128):
    index = lax.broadcasted_iota(jnp.int32, (8, lanes), 0)
    tile = jnp.zeros((8, lanes), F32)
    for k, row in enumerate(rows):
        tile = jnp.where(index == k, row, tile)
    return tile


def call(body, out, ins, scratch=(), mib=8, flops=1000000, hbm=(), any_=(), free=False):
    single = not isinstance(out, list)
    outs = [out] if single else list(out)
    ins = [pltpu.with_memory_space_constraint(x, pltpu.HBM) if k in hbm else x for k, x in enumerate(ins)]
    got = pl.pallas_call(
        body,
        out_shape=[pltpu.VMEM(s, d) if hbm and not free else jax.ShapeDtypeStruct(s, d) for s, d in outs],
        in_specs=[
            pl.BlockSpec(memory_space=pltpu.HBM if k in hbm else pl.ANY if k in any_ else pltpu.VMEM) for k in range(len(ins))
        ],
        out_specs=[pl.BlockSpec(memory_space=pltpu.VMEM)] * len(outs),
        scratch_shapes=list(scratch),
        compiler_params=pltpu.CompilerParams(vmem_limit_bytes=mib * MIB),
        cost_estimate=pl.CostEstimate(flops=flops, bytes_accessed=100000, transcendentals=0),
    )(*ins)
    return got[0] if single else got


def compress(
    rows, stream_hbm, gain_hbm, query_hbm, latent_hbm, rotary_hbm,
    out_ref, stream_ref, gain_ref, query_ref, latent_ref, rotary_ref, sems,
):
    copies = [
        pltpu.make_async_copy(a, b, sems.at[k])
        for k, (a, b) in enumerate((
            (stream_hbm, stream_ref), (gain_hbm, gain_ref), (rotary_hbm, rotary_ref),
            (latent_hbm, latent_ref), (query_hbm, query_ref),
        ))
    ]
    for copy in copies:
        copy.start()
    for copy in copies:
        copy.wait()
    own_f = mm_nt(diagonal(rows, rows).astype(BF16), stream_ref[...])
    scaled = (own_f * gain_ref[...]).astype(BF16)
    query = mm(scaled, query_ref[...])
    latent = mm(scaled, latent_ref[...])
    rotary = mm(scaled, rotary_ref[...]).astype(BF16)
    wide = rotary.shape[1]
    turned = mm_nt(diagonal(wide, wide).astype(BF16), rotary)
    square = jnp.broadcast_to(as_row(jnp.sum(own_f * own_f, axis=1, keepdims=True)), (8, 128)).astype(BF16)
    chunks = out_ref.shape[0]
    piece = wide // chunks
    for j in range(chunks):
        at = 128 * j
        part = query[:, at : at + 128] if at < query.shape[1] else latent[:, at - query.shape[1] : at - query.shape[1] + 128]
        out_ref[j, :rows, :] = part.astype(BF16)
        out_ref[j, rows:, :] = square
        out_ref[j, rows : rows + piece, :rows] = turned[piece * j : piece * (j + 1), :].astype(BF16)


def total_of(in_ref):
    total = in_ref[0].astype(F32)
    for p in range(1, in_ref.shape[0]):
        total += in_ref[p].astype(F32)
    return total


def plain_sum(in_ref, *refs):
    out_ref = refs[-1]
    total = total_of(in_ref).astype(BF16)
    for k in range(out_ref.shape[0]):
        out_ref[k] = total


def pack(part, token_ref, gate_hbm, up_hbm, down_hbm, gain_hbm, *refs):
    outs, gain_ref, sems = refs[:-2], refs[-2], refs[-1]
    count = len(outs)
    tiles = gate_hbm.shape[1] // 128
    high = gate_hbm.shape[0]
    top = 2 * part * high
    here = lax.axis_index(ALONG_Y)
    copies = []
    own_gain = pltpu.make_async_copy(gain_hbm, gain_ref, sems.at[sems.shape[0] - 1])
    own_gain.start()
    for k, out in enumerate(outs):
        for t in range(part):
            tile = jnp.minimum(part * ((here + k) % count) + t, tiles - 1)
            at = pl.ds(pl.multiple_of(128 * tile, 128), 128)
            for source, start in (
                (gate_hbm.at[:, at], high * t), (up_hbm.at[:, at], high * (part + t)), (down_hbm.at[at, :], top + 128 * t),
            ):
                copies.append(pltpu.make_async_copy(
                    source, out.at[start : start + source.shape[0], :], sems.at[len(copies)]
                ))
    for copy in copies:
        copy.start()
    own_gain.wait()
    tile = stacked(parts_of(gain_ref[...], 3)).astype(BF16)
    for out in outs:
        out[top + 128 * part :, :] = tile
    for copy in copies:
        copy.wait()
    for k, out in enumerate(outs):
        for t in range(part):
            @pl.when(part * ((here + k) % count) + t >= tiles)
            def _():
                for start in (high * t, high * (part + t)):
                    out[start : start + high, :] = jnp.zeros((high, 128), BF16)
                out[top + 128 * t : top + 128 * (t + 1), :] = jnp.zeros((128, 128), BF16)


def attend(
    rows, width, scale,
    in_ref, qgain_ref, lgain_ref, trig_ref,
    content_ref, rotary_ref, key_ref, value_ref, turned_ref, latents_ref,
    out_ref, q_ref, qt_ref, s_ref, w_ref, r_ref,
):
    heads = key_ref.shape[0]
    extent = turned_ref.shape[1]
    half = extent // 2
    pieces = q_ref.shape[0]
    chunks = in_ref.shape[0]
    n_query = qgain_ref.shape[0]
    eye = diagonal(rows, 128)
    part = extent // chunks
    first_row = lax.rsqrt(in_ref[0, rows + part : rows + part + 1, :].astype(F32) / width + EPS)
    first = as_col(first_row, rows)

    def normed_of(tiles, gain_ref):
        tiles = [in_ref[j, :rows, :].astype(F32) * first for j in tiles]
        square = jnp.sum(sum(x * x for x in tiles), axis=1, keepdims=True)
        inverse = lax.rsqrt(square / (128 * len(tiles)) + EPS)
        return jnp.concatenate([x * inverse * gain_ref[j : j + 1, :] for j, x in enumerate(tiles)], axis=1).astype(BF16)

    normed = normed_of(range(n_query), qgain_ref)
    row = normed_of(range(n_query, chunks), lgain_ref).astype(F32)
    for j in range(chunks):
        r_ref[part * j : part * (j + 1), :] = in_ref[j, rows : rows + part, :].astype(F32) * first_row
    low_half, high_half = r_ref[:half, :], r_ref[half:extent, :]
    cos_t, sin_t = trig_ref[:half, :], trig_ref[half : 2 * half, :]
    spun = jnp.concatenate([low_half * cos_t - high_half * sin_t, high_half * cos_t + low_half * sin_t], axis=0).astype(BF16)

    plain = mm(normed, content_ref[...]).astype(BF16)
    turn = mm(normed, rotary_ref[...])
    lane = lax.broadcasted_iota(jnp.int32, turn.shape, 1)
    across = turn.shape[1]
    swapped = jnp.where(lane % extent < half, pltpu.roll(turn, across - half, 1), pltpu.roll(turn, half, 1))
    turn = (turn * trig_ref[2 * half : 2 * half + 1, :] + swapped * trig_ref[2 * half + 1 : 2 * half + 2, :]).astype(BF16)
    turn_f = turn.astype(F32)

    q_ref[...] = jnp.zeros_like(q_ref)
    qt_ref[...] = jnp.zeros_like(qt_ref)
    own = []
    for h in range(heads):
        absorbed = mm(plain[:, 128 * h : 128 * h + 128], key_ref[h]).astype(BF16).astype(F32)
        for c in range(pieces):
            q_ref[c, pl.ds(h, rows, 8), :] = absorbed[:, 128 * c : 128 * c + 128]
        qt_ref[pl.ds(h, rows, 8), :] = turn_f if h == 0 else pltpu.roll(turn_f, across - extent * h, 1)
        turned_h = turn[:, extent * h : extent * (h + 1)]
        cross = jnp.sum(jnp.where(eye, mm(turned_h, spun), 0.0), axis=1, keepdims=True)
        own.append((jnp.sum(absorbed * row, axis=1, keepdims=True) + cross) * scale)

    for b in range(rows):
        at = slice(8 * b, 8 * b + 8)
        asked = jnp.concatenate([q_ref[c, at, :] for c in range(pieces)], axis=1).astype(BF16)
        s_ref[at, :] = (mm_nt(asked, latents_ref[b]) + mm(qt_ref[at, :extent].astype(BF16), turned_ref[b])) * scale
    scores = s_ref[...]
    tops = jnp.max(scores, axis=1, keepdims=True)
    expo = jnp.exp(scores - tops)
    s_ref[...] = expo
    r_ref[: 8 * rows, :] = jnp.broadcast_to(tops, (8 * rows, 128))
    r_ref[8 * rows :, :] = jnp.broadcast_to(jnp.sum(expo, axis=1, keepdims=True), (8 * rows, 128))
    for b in range(rows):
        at = slice(8 * b, 8 * b + 8)
        weighted = mm(s_ref[at, :].astype(BF16), latents_ref[b])
        for c in range(pieces):
            w_ref[c, at, :] = weighted[:, 128 * c : 128 * c + 128]

    here = lax.axis_index(KV) == 0
    values, logs = [], []
    for h in range(heads):
        weighted = jnp.concatenate([w_ref[c, pl.ds(h, rows, 8), :] for c in range(pieces)], axis=1)
        top = r_ref[pl.ds(h, rows, 8), :][:, :1]
        total = r_ref[pl.ds(8 * rows + h, rows, 8), :][:, :1]
        mine = jnp.where(here, own[h], -1e30)
        peak = jnp.maximum(top, mine)
        keep = jnp.exp(top - peak)
        add = jnp.exp(mine - peak)
        total = total * keep + add
        mixed = ((weighted * keep + row * add) / total).astype(BF16)
        values.append(mm(mixed, value_ref[h]).astype(BF16))
        logs += parts_of(as_row(peak + jnp.log(total)), 3)
    tile = stacked(logs).astype(BF16)
    for k in range(out_ref.shape[0]):
        for h in range(heads):
            out_ref[k, rows * h : rows * (h + 1), :] = values[h]
        out_ref[k, rows * heads :, :] = tile


def project(rows, in_ref, gain_ref, weight_ref, stream_ref, *refs):
    out_ref = refs[-1]
    blocks = in_ref.shape[0]
    heads = in_ref.shape[1] // rows
    logs = []
    for k in range(blocks):
        tile = in_ref[k, rows * heads :, :].astype(F32)
        logs.append(tile + pltpu.roll(tile, 7, 0) + pltpu.roll(tile, 6, 0))
    peak = functools.reduce(jnp.maximum, logs)
    factors = [jnp.exp(x - peak) for x in logs]
    whole = 1.0 / functools.reduce(jnp.add, factors)
    spread = jnp.concatenate([x * whole for x in factors], axis=0)
    eye = diagonal(rows, 128).astype(BF16)
    columns = sum(mm_nt(eye, x.astype(BF16)) for x in parts_of(spread, 2))
    values = []
    for h in range(heads):
        total = jnp.zeros((rows, 128), F32)
        for k in range(blocks):
            total += columns[:, 8 * k + 3 * h : 8 * k + 3 * h + 1] * in_ref[k, rows * h : rows * (h + 1), :].astype(F32)
        values.append(total.astype(BF16).astype(F32))
    values = jnp.concatenate(values, axis=1)
    square = as_row(jnp.sum(values * values, axis=1, keepdims=True))
    scaled = (values * gain_ref[...]).astype(BF16)
    product = mm(scaled, weight_ref[...]).astype(BF16)
    tile = stacked(parts_of(square, 2))
    own = mm_nt(diagonal(rows, rows).astype(BF16), stream_ref[...])
    count = own.shape[1]
    place = (count, 128)
    for g in range(rows // 8):
        at = lax.broadcasted_iota(jnp.int32, place, 0) + SPOT + count * g == lax.broadcasted_iota(jnp.int32, place, 1)
        tile += mm(own[8 * g : 8 * g + 8, :].astype(BF16), at.astype(BF16))
    tile = tile.astype(BF16)
    for p in range(out_ref.shape[0]):
        out_ref[p, :rows, :] = product
        out_ref[p, rows:, :] = tile


def expand(rows, count, part, width, in_ref, *refs):
    packed_refs, out_ref, middle_ref = refs[:-2], refs[-2], refs[-1]
    blocks = len(packed_refs)
    peers = in_ref.shape[0] // blocks
    heads = sum(in_ref[p, rows:, :].astype(F32) for p in range(peers))
    head_col = as_col(lax.rsqrt((heads[0:1, :rows] + heads[1:2, :rows]) / width + EPS), rows)
    owner = lax.broadcasted_iota(jnp.int32, (8, 128), 1) // count
    top = packed_refs[0].shape[0] - 8
    here = lax.axis_index(ALONG_Y)
    square = jnp.zeros((rows, 1), F32)
    scaled = []
    for k in range(blocks):
        y = (here + blocks - k) % blocks
        group = [in_ref[peers * y + p].astype(F32) for p in range(peers)]
        attended = functools.reduce(jnp.add, [x[:rows] for x in group])
        stream = []
        for g in range(rows // 8):
            piece = jnp.zeros((8, 128), F32)
            for p, x in enumerate(group):
                piece = jnp.where(owner == p, pltpu.roll(x[rows:], (count * (p - g) - SPOT) % 128, 1), piece)
            stream.append(piece)
        middle = (jnp.concatenate(stream, axis=0) + head_col * attended).astype(BF16).astype(F32)
        square += jnp.sum(middle * middle, axis=1, keepdims=True)
        if k == 0:
            middle_ref[...] = middle.astype(BF16)
        gain = packed_refs[k][top:, :].astype(F32)
        scaled.append((middle * (gain[0:1] + gain[1:2] + gain[2:3])).astype(BF16))
    products = [
        sum(mm(scaled[k], packed_refs[k][128 * t : 128 * t + 128, :]) for k in range(blocks)).astype(BF16)
        for t in range(2 * part)
    ]
    tile = stacked(parts_of(as_row(square), 2)).astype(BF16)
    for k in range(out_ref.shape[0]):
        for t, product in enumerate(products):
            out_ref[k, rows * t : rows * (t + 1), :] = product
        out_ref[k, 2 * part * rows :, :] = tile


def contract(rows, part, width, in_ref, *refs):
    packed_refs, out_ref = refs[:-1], refs[-1]
    total = total_of(in_ref)
    last = 2 * part * rows
    scale = as_col(lax.rsqrt((total[last : last + 1, :] + total[last + 1 : last + 2, :]) / width + EPS), rows)
    hidden = []
    for t in range(part):
        gate = total[rows * t : rows * (t + 1)] * scale
        up = total[rows * (part + t) : rows * (part + t + 1)] * scale
        hidden.append((gate / (1.0 + jnp.exp(-gate)) * up).astype(BF16))
    hidden = jnp.concatenate(hidden, axis=1)
    blocks = len(packed_refs)
    peers = out_ref.shape[0] // blocks
    here = lax.axis_index(ALONG_Y)
    top = packed_refs[0].shape[0] - 8 - 128 * part
    for k, packed_ref in enumerate(packed_refs):
        y = (here + blocks - k) % blocks
        product = mm(hidden, packed_ref[top : top + 128 * part, :]).astype(BF16)
        for p in range(peers):
            out_ref[peers * y + p] = product


def finish(in_ref, middle_ref, out_ref):
    total = (middle_ref[...].astype(F32) + total_of(in_ref)).astype(BF16)
    width = out_ref.shape[0]
    at = (width, total.shape[1])
    row = lax.broadcasted_iota(jnp.int32, at, 0) + width * lax.axis_index(TP)
    pick = (row == lax.broadcasted_iota(jnp.int32, at, 1)).astype(BF16)
    out_ref[...] = mm_nt(pick, total).astype(BF16)


def exchange(x, axis):
    return lax.all_to_all(x, axis, 0, 0, tiled=True)


def local(
    stream, attention_gain, query_down, latent_down, rotary_down, query_gain, latent_gain,
    query_content, query_rotary, key_absorb, value_absorb, latent_cache, rotary_cache,
    head_gain, output_weight, mixer_gain, gate_weight, up_weight, down_weight,
):
    kv, tp = lax.axis_size(KV), lax.axis_size(TP)
    near, far = lax.axis_size(NEAR), lax.axis_size(FAR)
    rows, count = stream.shape
    width = count * kv * tp
    heads, nope, latent = key_absorb.shape
    rope = rotary_cache.shape[2]
    block_len = latent_cache.shape[1]
    position = block_len * kv
    scale = (nope + rope) ** (-0.5)
    ys, zs = lax.axis_size(ALONG_Y), lax.axis_size("z")
    part = -(-gate_weight.shape[1] // 128 // ys)
    angle = position * BASE ** (-np.arange(rope // 2) * 2.0 / rope)
    cos, sin = np.cos(angle), np.sin(angle)
    trig = np.concatenate([
        np.tile(cos[:, None], (1, 128)), np.tile(sin[:, None], (1, 128)),
        np.tile(np.concatenate([cos, cos]), heads)[None], np.tile(np.concatenate([-sin, sin]), heads)[None],
        np.zeros((6, 128)),
    ])
    trig = jnp.asarray(trig, F32)
    lines = rows + 8

    sources = (stream.T, attention_gain[None], query_down, latent_down, rotary_down)
    sent = call(
        functools.partial(compress, rows), ((near, lines, 128), BF16), sources,
        scratch=[pltpu.VMEM(x.shape, x.dtype) for x in sources] + [pltpu.SemaphoreType.DMA((len(sources),))],
        hbm=range(len(sources)),
    )
    packed = call(
        functools.partial(pack, part),
        [((2 * part * gate_weight.shape[0] + 128 * part + 8, 128), BF16)] * ys,
        (sent, gate_weight, up_weight, down_weight, mixer_gain[None]),
        scratch=[pltpu.VMEM((1, 128), F32), pltpu.SemaphoreType.DMA((3 * part * ys + 1,))], hbm=(1, 2, 3, 4), flops=WAIT // 10, any_=(0,), free=True,
    )
    packed = [packed[0]] + [
        lax.ppermute(packed[k], ALONG_Y, [(y, (y + k) % ys) for y in range(ys)]) for k in range(1, ys)
    ]
    sent = call(
        plain_sum, ((far, lines, 128), BF16), (exchange(sent, NEAR), *packed[:1]), flops=WAIT, any_=(1,),
    )
    sources = (
        query_gain.reshape(-1, 128), latent_gain.reshape(-1, 128), trig,
        query_content, query_rotary, key_absorb, value_absorb, jnp.swapaxes(rotary_cache, 1, 2),
    )
    sent = call(plain_sum, ((near, lines, 128), BF16), (exchange(sent, FAR),), flops=WAIT)
    sent = call(
        functools.partial(attend, rows, width, scale), ((kv, rows * heads + 8, 128), BF16),
        (exchange(sent, NEAR), *sources, latent_cache),
        scratch=[
            pltpu.VMEM((latent // 128, 8 * rows, 128), F32), pltpu.VMEM((8 * rows, heads * rope), F32),
            pltpu.VMEM((8 * rows, block_len), F32), pltpu.VMEM((latent // 128, 8 * rows, 128), F32),
            pltpu.VMEM((16 * rows, 128), F32),
        ],
    )
    sent = call(
        functools.partial(project, rows), ((ys * tp, lines, 128), BF16),
        (exchange(sent, ALONG_KV), head_gain[None], output_weight, stream.T, *packed[1:]), any_=range(4, 3 + ys),
    )
    sent, middle = call(
        functools.partial(expand, rows, count, part, head_gain.shape[0] * tp),
        [((zs, 2 * part * rows + 8, 128), BF16), ((rows, 128), BF16)],
        (exchange(sent, ALONG_Y + TP), *packed),
    )
    sent = call(
        functools.partial(contract, rows, part, width), ((ys * tp, rows, 128), BF16),
        (exchange(sent, "z"), *packed),
    )
    return call(finish, ((count, rows), BF16), (exchange(sent, ALONG_Y + TP), middle)).T


def solution(mesh):
    grid = Mesh(mesh.devices.reshape(mesh.shape["kv"] // 4, 2, 2, mesh.shape["tp"] // 2, 2), KV + TP)
    both = KV + TP
    return jax.shard_map(
        local,
        mesh=grid,
        in_specs=(
            P(None, both), P(both), P(both, None), P(both, None), P(both, None), P(), P(),
            P(None, TP), P(None, TP), P(TP, None, None), P(TP, None, None),
            P(None, KV, None), P(None, KV, None), P(TP), P(TP, KV), P(KV),
            P(KV, TP), P(KV, TP), P(TP, KV),
        ),
        out_specs=P(None, both),
        check_vma=False,
    )
```
